32 devices in a mesh: ep: 8 (over z, x), tp: 4 (over y, core).
Axes of the slice: x: 2, y: 2, z: 4, core: 2. Of those that a mesh axis runs over, the one named last changes fastest.
Arguments:
- mix_input: bfloat16 [3072, 2048], P('ep', 'tp'), may hold values from -6 to 6
- mix_gain: float32 [2048], replicated, may hold values from 0.1 to 1.9
- gate_b_weight: bfloat16 [2048, 2048], P(None, 'tp'), may hold values from -0.125 to 0.125
- gate_c_weight: bfloat16 [2048, 2048], P(None, 'tp'), may hold values from -0.125 to 0.125
- value_weight: bfloat16 [2048, 2048], P(None, 'tp'), may hold values from -0.125 to 0.125
- conv_weight: float32 [3, 2048], P(None, 'tp'), may hold values from -3 to 3
- out_weight: bfloat16 [2048, 2048], P('tp'), may hold values from -0.125 to 0.125
- expert_input: bfloat16 [1280, 2048], P('ep', 'tp'), may hold values from -6 to 6
- expert_gain: float32 [2048], replicated, may hold values from 0.1 to 1.9
- routes: int32 [1280, 2], P('ep'), may hold values from 0 to 7, all different within a row; in each aligned block of 160 rows (0 to 159, 160 to 319, ...) at most 80 rows name the same one
- route_weight: float32 [1280, 2], P('ep'), may hold values from 0.2 to 1
- expert_gate: bfloat16 [8, 2048, 3072], P('ep', None, 'tp'), may hold values from -0.125 to 0.125
- expert_up: bfloat16 [8, 2048, 3072], P('ep', None, 'tp'), may hold values from -0.125 to 0.125
- expert_down: bfloat16 [8, 3072, 2048], P('ep', 'tp'), may hold values from -0.109375 to 0.109375
Outputs:
- mix_output: bfloat16 [3072, 2048], P('ep', 'tp')
- expert_output: bfloat16 [1280, 2048], P('ep', 'tp')
The draws below stay inside these ranges and needn't reach their ends.
Inputs may be any that keep to these rules, and one draw needn't show every extreme that they name: `routes`: the 2 experts of a row differ. Among the rows of one device no expert is named more than 80 times, a bound that some block reaches.
All inputs are finite; a program needn't handle non-finite values.
Results may differ from the reference program's by a relative error of at most 0.019.
Values may be sent and summed in bfloat16 or wider, within the bound.
A program may use at most 64 MiB of HBM per device.

```python
import math
import jax
import jax.numpy as jnp
import numpy as np
from jax import lax

D = 2048
FF = 3072
TOPK = 2
TOK_B = 160
EXPERTS = 8
CAP = 80
TOKENS_A = 3072
TOKENS_B = 1280
N_EP = 8
N_TP = 4


def levels(own_key, dims, split, low, high):
    def one(position, parts):
        draws = jax.random.uniform(jax.random.fold_in(jax.random.fold_in(own_key, 6), position), (parts,), jnp.float32, low / len(split), high / len(split))
        return jnp.repeat(jnp.exp(draws), dims[position] // parts).reshape((-1,) + (1,) * (len(dims) - position - 1))

    factor_of = one(*split[0])
    for cut in split[1:]:
        factor_of = factor_of * one(*cut)
    return factor_of


def shared_out(stream_key, own, number, rows, count, top, bound, slope):
    ranking = jax.random.permutation(stream_key, count)
    packed, common = load_shares(count, rows * top, bound, slope, True), load_shares(count, rows * top, bound, slope, False)
    places = jnp.arange(count)

    def named(tallies, rotation):
        used = int((tallies > 0).sum())
        fixed = max(1, used // 4)
        passed = fixed + (places - fixed + rotation * (used - fixed)) % max(1, count - fixed)
        return jnp.zeros((count,), jnp.int32).at[ranking[jnp.where(places < fixed, places, passed)]].set(jnp.asarray(tallies, jnp.int32))

    tallies = jnp.where(number % 4 == 0, named(packed, number // 4), named(common, number - number // 4 - 1))
    mixed = jax.random.permutation(jax.random.fold_in(own, 3), count)
    donor, receiver = mixed[0:count // 2 * 2:2], mixed[1:count // 2 * 2:2]
    margin = jnp.minimum(tallies[donor] - 1, bound - tallies[receiver]) // 2
    margin = jnp.where((donor == ranking[0]) | (receiver == ranking[0]) | (tallies[receiver] == 0), 0, jnp.maximum(margin, 0))
    passed = jax.random.randint(jax.random.fold_in(own, 4), (count // 2,), 0, 1 << 20) % (margin + 1)
    tallies = tallies.at[donor].add(-passed).at[receiver].add(passed)
    members = jnp.searchsorted(jnp.cumsum(tallies), jnp.arange(rows * top), side="right").astype(jnp.int32)
    listing = members.reshape(top, rows).T
    listing = listing[jax.random.permutation(jax.random.fold_in(own, 1), rows)]
    rotation = jax.random.randint(jax.random.fold_in(own, 2), (rows, 1), 0, top)
    return jnp.take_along_axis(listing, (jnp.arange(top)[None, :] + rotation) % top, axis=1)


def load_shares(number_of, total, bound, slope, full):
    weights = [(1 << 20) // math.isqrt(standing ** slope) + 1 for standing in range(1, number_of + 1)]
    largest = bound if full else min(bound, max(-(-total // number_of), total * weights[0] // sum(weights)))
    least = 1 if total - largest >= number_of - 1 else 0
    counts, rest = [largest] + [least] * (number_of - 1), total - largest - least * (number_of - 1)
    while rest > 0:
        candidates = [i for i in range(1, number_of) if counts[i] < largest] or [i for i in range(1, number_of) if counts[i] < bound]
        mass, left = sum([weights[i] for i in candidates]), rest
        for i in candidates:
            more = min(bound - counts[i], max(1, left * weights[i] // mass), rest)
            counts[i] = counts[i] + more
            rest = rest - more
    return np.array(counts)


def centred(own_key, shape, scale, reach, pieces=(), kind=jnp.bfloat16):
    drawn = scale * jax.random.normal(own_key, shape, jnp.float32)
    if pieces:
        drawn = drawn * levels(own_key, shape, pieces, -0.22, 0.18)
    return jnp.clip(drawn, -reach, reach).astype(kind)


def setup_inputs(seed: int = 0) -> dict:
    splits = jax.random.split(jax.random.key(seed), 15)
    mix_input = centred(splits[0], (TOKENS_A, D), 1.0, 6.0, ((0, 8), (1, 4)))
    mix_gain = jnp.clip(1.0 + 0.18 * jax.random.normal(splits[1], (D,), jnp.float32), 0.1, 1.9)
    gate_b_weight = centred(splits[2], (D, D), D ** -0.5, 0.125, ((1, 4),))
    gate_c_weight = centred(splits[3], (D, D), D ** -0.5, 0.125, ((1, 4),))
    value_weight = centred(splits[4], (D, D), D ** -0.5, 0.125, ((1, 4),))
    conv_weight = centred(splits[5], (3, D), 0.6, 3.0, ((1, 4),), jnp.float32)
    out_weight = centred(splits[6], (D, D), D ** -0.5, 0.125, ((0, 4),))
    expert_input = centred(splits[7], (TOKENS_B, D), 1.0, 6.0, ((0, 8), (1, 4)))
    expert_gain = jnp.clip(1.0 + 0.18 * jax.random.normal(splits[8], (D,), jnp.float32), 0.1, 1.9)
    routes_keys = jax.random.split(jax.random.fold_in(splits[9], 1), TOKENS_B // TOK_B)
    routes_turns = jax.random.permutation(jax.random.fold_in(splits[9], 3), TOKENS_B // TOK_B)
    routes = jax.vmap(lambda own, number: shared_out(jax.random.fold_in(splits[9], 2), own, number, TOK_B, EXPERTS, TOPK, CAP, 1))(routes_keys, routes_turns).reshape((TOKENS_B, TOPK))
    route_weight = jnp.clip(jnp.exp(math.log(1.0) - 1.609438 * jax.random.uniform(splits[10], (TOKENS_B, TOPK), jnp.float32) ** levels(splits[10], (TOKENS_B, TOPK), ((0, 8),), -0.2, 0.2)), 0.2, 1.0)
    expert_gate = centred(splits[11], (EXPERTS, D, FF), D ** -0.5, 0.125, ((0, 8), (2, 4)))
    expert_up = centred(splits[12], (EXPERTS, D, FF), D ** -0.5, 0.125, ((0, 8), (2, 4)))
    expert_down = centred(splits[13], (EXPERTS, FF, D), FF ** -0.5, 0.109375, ((0, 8), (1, 4)))
    return {"mix_input": mix_input, "mix_gain": mix_gain, "gate_b_weight": gate_b_weight, "gate_c_weight": gate_c_weight, "value_weight": value_weight, "conv_weight": conv_weight, "out_weight": out_weight, "expert_input": expert_input, "expert_gain": expert_gain, "routes": routes, "route_weight": route_weight, "expert_gate": expert_gate, "expert_up": expert_up, "expert_down": expert_down}


epsilon = 1e-06
routed_scale = 2.5

def norm_project(source, gain_vector, matrices):
    widened = source.astype(jnp.float32)
    factor = lax.rsqrt(lax.optimization_barrier(jnp.mean(widened * widened, axis=-1, keepdims=True)) + epsilon)
    scaled = (widened * gain_vector).astype(jnp.bfloat16)
    return [jnp.dot(scaled, matrix, preferred_element_type=jnp.float32) * factor for matrix in matrices]

def block_sum(operand, weights):
    span_size = operand.shape[1] // N_TP
    running = jnp.zeros((operand.shape[0], weights.shape[1]), jnp.float32)
    for block_index in range(N_TP):
        low = block_index * span_size
        partial_value = jnp.dot(operand[:, low:low + span_size], weights[low:low + span_size], preferred_element_type=jnp.float32)
        running = running + partial_value.astype(jnp.bfloat16).astype(jnp.float32)
    return running.astype(jnp.bfloat16)

def reference(mix_input, mix_gain, gate_b_weight, gate_c_weight, value_weight, conv_weight, out_weight, expert_input, expert_gain, routes, route_weight, expert_gate, expert_up, expert_down):
    outer_gate, inner_gate, conv_values = norm_project(mix_input, mix_gain, (gate_b_weight, gate_c_weight, value_weight))
    product = inner_gate * conv_values
    seq_length = product.shape[0]
    padded = jnp.concatenate([jnp.zeros((2, product.shape[1]), jnp.float32), product], axis=0)
    convolved = conv_weight[0] * padded[:seq_length] + conv_weight[1] * padded[1:seq_length + 1] + conv_weight[2] * padded[2:]
    gated = (outer_gate * convolved).astype(jnp.bfloat16)
    mix_output = block_sum(gated, out_weight)
    flat_routes = routes.reshape(-1).astype(jnp.int32)
    pair_count = flat_routes.shape[0]
    slot_count = N_EP * CAP
    expert_ids = jnp.arange(EXPERTS, dtype=jnp.int32)
    matches = (flat_routes[:, None] == expert_ids[None, :]).astype(jnp.int32)
    ranks = lax.optimization_barrier(jnp.sum((jnp.cumsum(matches, axis=0) - matches) * matches, axis=1)).astype(jnp.int32)
    owners_all = (jnp.arange(pair_count, dtype=jnp.int32) // TOPK).astype(jnp.int32)

    def one_expert(inputs):
        gate_matrix, up_matrix, down_matrix, expert_id = inputs
        chosen = flat_routes == expert_id
        target = jnp.where(chosen, ranks, slot_count).astype(jnp.int32)
        owners = jnp.zeros((slot_count,), jnp.int32).at[target].set(owners_all, mode='drop')
        gathered = expert_input[owners]
        hidden_gate, hidden_up = norm_project(gathered, expert_gain, (gate_matrix, up_matrix))
        activated = (jax.nn.silu(hidden_gate) * hidden_up).astype(jnp.bfloat16)
        return block_sum(activated, down_matrix)
    results = lax.map(one_expert, (expert_gate, expert_up, expert_down, expert_ids))
    picked = results[flat_routes, ranks].astype(jnp.float32).reshape(routes.shape[0], TOPK, -1)
    normalized = route_weight / lax.optimization_barrier(jnp.sum(route_weight, axis=1, keepdims=True)) * routed_scale
    expert_output = lax.optimization_barrier(jnp.sum(picked * normalized[:, :, None], axis=1)).astype(jnp.bfloat16)
    return (mix_output, expert_output)
```

```python
import functools

import jax
import jax.numpy as jnp
from jax import lax
from jax.experimental import pallas as pl
from jax.experimental.pallas import tpu as pltpu
from jax.sharding import PartitionSpec as P

MESH = pl.DeviceIdType.MESH
epsilon = 1e-06
routed_scale = 2.5
f32 = jnp.float32
bf16 = jnp.bfloat16


def kernel(
    dims,
    mix_ref, mgain_ref, wb_hbm, wc_hbm, wv_hbm, conv_ref, wo_hbm,
    exp_ref, egain_ref, routes_ref, rw_ref, wg_hbm, wu_hbm, wd_hbm,
    mo_ref, eo_ref,
    wb, wc, wv, wo, wg, wu, wd, w_sem,
    tables, outg, xg, xs, fac, outer, prod, edge, gated, pm, rm, sm, ym,
    xe, xes, efac, act, pe, re, se, yr, fin, ret,
    mys, myr, mps, mpr, eps, epr, eys, eyr, pps, ppr, edges,
    rms, rmr, yms, ymr, res, rer, ses, ser, rts, rtr,
):
    n_ep, n_tp, cap, group = dims
    chips = n_tp // 2
    n_group = n_ep // group
    rows, feat = mix_ref.shape
    width = feat * n_tp
    tok = exp_ref.shape[0]
    slots = n_ep * cap
    e = lax.axis_index("ep")
    t = lax.axis_index("tp")
    y, c = lax.div(t, 2), lax.rem(t, 2)
    partner = y * 2 + 1 - c
    home = lax.div(e, group)

    def cols(b):
        return pl.ds(pl.multiple_of(b * feat, feat), feat)

    def remote(src, dst, send_sem, recv_sem, ep, tp):
        return pltpu.make_async_remote_copy(
            src_ref=src, dst_ref=dst, send_sem=send_sem, recv_sem=recv_sem,
            device_id=(ep, tp), device_id_type=MESH,
        )

    def ahead(dy):
        return lax.rem(y + dy, chips) * 2 + c

    def behind(dy):
        return lax.rem(y - dy + chips, chips) * 2 + c

    def loop(count, body):
        lax.fori_loop(0, count, lambda i, carry: (body(i), carry)[1], 0)

    def mix_y(dy):
        return remote(mix_ref, xg.at[:, cols(t)], mys.at[dy], myr.at[dy], e, ahead(dy))

    def mix_p():
        return remote(mix_ref, xg.at[:, cols(t)], mps.at[0], mpr.at[0], e, partner)

    def mix_f(dy):
        part = xg.at[:, cols(behind(dy))]
        return remote(part, part, mps.at[dy], mpr.at[dy], e, partner)

    def dispatch(d):
        s = lax.rem(e + d, n_ep)
        return remote(outg.at[s], xe.at[e, :, cols(t)], eps.at[d], epr.at[d], s, t)

    def span_in(i):
        return pl.ds(lax.rem(home - i + n_group, n_group) * group, group)

    def exp_y(i, dy):
        part = xe.at[span_in(i), :, cols(t)]
        return remote(part, part, eys.at[dy, i], eyr.at[dy, i], e, ahead(dy))

    def exp_p(i):
        part = xe.at[span_in(i), :, cols(t)]
        return remote(part, part, pps.at[0, i], ppr.at[0, i], e, partner)

    def exp_f(i, dy):
        part = xe.at[span_in(i), :, cols(behind(dy))]
        return remote(part, part, pps.at[dy, i], ppr.at[dy, i], e, partner)

    def edge_copy():
        return remote(
            prod.at[pl.ds(rows, 8)], edge, edges.at[0], edges.at[1], lax.rem(e + 1, n_ep), t
        )

    def mix_half(q):
        return remote(pm.at[q * 2 + 1 - c], rm.at[q], rms.at[q], rmr.at[q], e, partner)

    def mix_sum(dy):
        return remote(sm.at[dy], ym.at[dy], yms.at[dy], ymr.at[dy], e, ahead(dy))

    def exp_half(q):
        return remote(pe.at[q * 2 + 1 - c], re.at[q], res.at[q], rer.at[q], e, partner)

    def span_out(i):
        return pl.ds(lax.rem(home + 1 + i, n_group) * group, group)

    def exp_sum(i, dy):
        return remote(
            se.at[dy, span_out(i)], yr.at[dy, span_out(i)],
            ses.at[dy, i], ser.at[dy, i], e, ahead(dy),
        )

    def back(d):
        s = lax.rem(e + d, n_ep)
        return remote(fin.at[s], ret.at[e], rts.at[d], rtr.at[d], s, t)

    loads = [
        pltpu.make_async_copy(src, dst, w_sem.at[i])
        for i, (src, dst) in enumerate(
            ((wb_hbm, wb), (wc_hbm, wc), (wv_hbm, wv), (wo_hbm, wo),
             (wg_hbm, wg), (wu_hbm, wu), (wd_hbm, wd))
        )
    ]
    for load in loads:
        load.start()

    barrier = pltpu.get_barrier_semaphore()
    for dy in range(1, chips):
        pl.semaphore_signal(barrier, inc=1, device_id=(e, ahead(dy)), device_id_type=MESH)
    pl.semaphore_signal(barrier, inc=1, device_id=(e, partner), device_id_type=MESH)

    def greet(d):
        pl.semaphore_signal(
            barrier, inc=1, device_id=(lax.rem(e + d + 1, n_ep), t), device_id_type=MESH
        )

    loop(n_ep - 1, greet)

    lane = lax.broadcasted_iota(jnp.int32, (tok, 128), 1)
    named = [routes_ref[:, k : k + 1] == lane for k in range(2)]
    either = jnp.where(named[0] | named[1], 1.0, 0.0).astype(bf16)
    before = (
        lax.broadcasted_iota(jnp.int32, (tok, tok), 0)
        > lax.broadcasted_iota(jnp.int32, (tok, tok), 1)
    )
    counts = jnp.dot(
        jnp.where(before, 1.0, 0.0).astype(bf16), either, preferred_element_type=f32
    )
    slot_iota = lax.broadcasted_iota(jnp.int32, (tok, slots), 1).astype(f32)
    both = []
    for k in range(2):
        rank = jnp.sum(jnp.where(named[k], counts, 0.0), axis=1, keepdims=True)
        slot = routes_ref[:, k : k + 1].astype(f32) * float(cap) + rank
        one = jnp.where(slot_iota == slot, 1.0, 0.0)
        tables[k] = one.astype(bf16)
        both.append(one)
    send = (both[0] + both[1]).astype(bf16)
    outg[...] = (
        lax.dot_general(
            send, exp_ref[...], (((0,), (0,)), ((), ())), preferred_element_type=f32
        )
        .astype(bf16)
        .reshape(n_ep, cap, feat)
    )

    pl.semaphore_wait(barrier, n_ep - 1 + chips)

    loop(n_ep - 1, lambda d: dispatch(d + 1).start())
    for dy in range(1, chips):
        mix_y(dy).start()
    mix_p().start()
    xe[e, :, cols(t)] = outg[e]
    xg[:, cols(t)] = mix_ref[...]

    def pass_on(i):
        first = lax.rem(home - i + n_group, n_group) * group
        for j in range(group):
            d = lax.rem(e - first - j + n_ep, n_ep)

            @pl.when(d != 0)
            def _():
                dispatch(d).wait_recv()

        for dy in range(1, chips):
            exp_y(i, dy).start()
        exp_p(i).start()

    loop(n_group, pass_on)

    for dy in range(1, chips):
        mix_y(dy).wait_recv()
        mix_f(dy).start()
    mix_p().wait_recv()
    for dy in range(1, chips):
        mix_f(dy).wait_recv()

    tile = 32

    def scale_mix(i):
        at = pl.ds(pl.multiple_of(i * tile, tile), tile)
        x = xg[at].astype(f32)
        fac[at] = lax.rsqrt(jnp.sum(x * x, axis=1, keepdims=True) / width + epsilon)
        xs[at] = (x * mgain_ref[...]).astype(bf16)

    loop(rows // tile, scale_mix)
    for load in loads[:3]:
        load.wait()
    wide = 256 if feat % 256 == 0 else feat

    def project(i):
        at = pl.ds(pl.multiple_of(i * wide, wide), wide)
        x = xs[...]
        factor = fac[...]
        inner = jnp.dot(x, wc[:, at], preferred_element_type=f32) * factor
        values = jnp.dot(x, wv[:, at], preferred_element_type=f32) * factor
        prod[pl.ds(8, rows), at] = inner * values
        outer[:, at] = jnp.dot(x, wb[:, at], preferred_element_type=f32) * factor

    loop(feat // wide, project)
    edge_copy().start()
    edge_copy().wait_recv()
    prod[0:8] = jnp.where(e == 0, 0.0, edge[...])

    def convolve(i):
        at = pl.ds(pl.multiple_of(i * 128, 128), 128)
        convolved = (
            conv_ref[0:1, at] * prod[pl.ds(6, rows), at]
            + conv_ref[1:2, at] * prod[pl.ds(7, rows), at]
            + conv_ref[2:3, at] * prod[pl.ds(8, rows), at]
        )
        gated[:, at] = (outer[:, at] * convolved).astype(bf16)

    loop(feat // 128, convolve)
    loads[3].wait()

    def mix_down(b):
        pm[b] = jnp.dot(gated[...], wo[:, cols(b)], preferred_element_type=f32).astype(bf16)

    loop(n_tp, mix_down)
    for q in range(chips):
        mix_half(q).start()

    def relay(i):
        for dy in range(1, chips):
            exp_y(i, dy).wait_recv()
            exp_f(i, dy).start()

    for q in range(chips):
        mix_half(q).wait_recv()
    for dy in range(1, chips):
        q = lax.rem(y + dy, chips)
        sm[dy] = (pm[ahead(dy)].astype(f32) + rm[q].astype(f32)).astype(bf16)
        mix_sum(dy).start()
    loop(n_group, relay)

    def arrive(i):
        exp_p(i).wait_recv()
        for dy in range(1, chips):
            exp_f(i, dy).wait_recv()

    loop(n_group, arrive)

    def scale_exp(i):
        at = pl.ds(pl.multiple_of(i * cap, cap), cap)
        x = xe[i].astype(f32)
        efac[at] = lax.rsqrt(jnp.sum(x * x, axis=1, keepdims=True) / width + epsilon)
        xes[at] = (x * egain_ref[...]).astype(bf16)

    loop(n_ep, scale_exp)
    loads[4].wait()
    loads[5].wait()
    hidden = wd.shape[0]
    wide_h = 256 if hidden % 256 == 0 else hidden

    def activate(i):
        at = pl.ds(i * wide_h, wide_h) if wide_h == hidden else pl.ds(
            pl.multiple_of(i * wide_h, wide_h), wide_h
        )
        x = xes[...]
        gate = jnp.dot(x, wg[0, :, at], preferred_element_type=f32) * efac[...]
        up = jnp.dot(x, wu[0, :, at], preferred_element_type=f32) * efac[...]
        act[:, at] = (gate / (1.0 + jnp.exp(-gate)) * up).astype(bf16)

    if wide_h == hidden:
        x = xes[...]
        gate = jnp.dot(x, wg[0], preferred_element_type=f32) * efac[...]
        up = jnp.dot(x, wu[0], preferred_element_type=f32) * efac[...]
        act[...] = (gate / (1.0 + jnp.exp(-gate)) * up).astype(bf16)
    else:
        loop(hidden // wide_h, activate)
    loads[6].wait()

    def exp_down(b):
        out = jnp.dot(act[...], wd[:, cols(b)], preferred_element_type=f32)
        pe[b] = out.astype(bf16).reshape(n_ep, cap, feat)

    loop(n_tp, exp_down)
    for q in range(chips):
        exp_half(q).start()

    for q in range(chips):
        exp_half(q).wait_recv()

    def push(i):
        at = span_out(i)
        for dy in range(1, chips):
            q = lax.rem(y + dy, chips)
            se[dy, at] = (pe[ahead(dy), at].astype(f32) + re[q, at].astype(f32)).astype(bf16)
            exp_sum(i, dy).start()

    loop(n_group, push)

    total = pm[t].astype(f32) + rm[y].astype(f32)
    for dy in range(1, chips):
        mix_sum(dy).wait_recv()
        total = total + ym[dy].astype(f32)
    mo_ref[...] = total.astype(bf16)

    def finish(i):
        at = span_out(i)
        whole = pe[t, at].astype(f32) + re[y, at].astype(f32)
        for dy in range(1, chips):
            exp_sum(i, dy).wait_recv()
            whole = whole + yr[dy, at].astype(f32)
        fin[at] = whole.astype(bf16)
        first = lax.rem(home + 1 + i, n_group) * group
        for j in range(group):
            d = lax.rem(first + j - e + n_ep, n_ep)

            @pl.when(d != 0)
            def _():
                back(d).start()

    loop(n_group, finish)
    ret[e] = fin[e]
    loop(n_ep - 1, lambda d: back(d + 1).wait_recv())

    scores = rw_ref[...]
    normalized = scores / jnp.sum(scores, axis=1, keepdims=True) * routed_scale
    results = ret[...].reshape(slots, feat)
    eo_ref[...] = (
        normalized[:, 0:1] * jnp.dot(tables[0], results, preferred_element_type=f32)
        + normalized[:, 1:2] * jnp.dot(tables[1], results, preferred_element_type=f32)
    ).astype(bf16)

    def drain(d):
        dispatch(d + 1).wait_send()
        back(d + 1).wait_send()

    loop(n_ep - 1, drain)
    mix_p().wait_send()
    edge_copy().wait_send()
    for dy in range(1, chips):
        mix_y(dy).wait_send()
        mix_f(dy).wait_send()
        mix_sum(dy).wait_send()
    for q in range(chips):
        mix_half(q).wait_send()
        exp_half(q).wait_send()

    def drain_groups(i):
        exp_p(i).wait_send()
        for dy in range(1, chips):
            exp_y(i, dy).wait_send()
            exp_f(i, dy).wait_send()
            exp_sum(i, dy).wait_send()

    loop(n_group, drain_groups)


def solution(mesh):
    n_ep, n_tp = mesh.shape["ep"], mesh.shape["tp"]
    chips = n_tp // 2

    def local(
        mix_input, mix_gain, gate_b, gate_c, value_w, conv_weight, out_weight,
        expert_input, expert_gain, routes, route_weight, expert_gate, expert_up, expert_down,
    ):
        rows, feat = mix_input.shape
        width = feat * n_tp
        tok, top = routes.shape
        experts = n_ep * expert_gate.shape[0]
        assert expert_gate.shape[0] == 1 and top == 2
        cap = -(-(2 * tok * top // experts) // 16) * 16
        hidden = expert_gate.shape[2]
        group = max(1, n_ep // 8)
        n_group = n_ep // group
        slots = n_ep * cap
        vm, sem = pltpu.VMEM, pltpu.SemaphoreType.DMA
        scratch = [
            vm((width, feat), bf16), vm((width, feat), bf16), vm((width, feat), bf16),
            vm((feat, width), bf16),
            vm((1, width, hidden), bf16), vm((1, width, hidden), bf16), vm((hidden, width), bf16),
            sem((7,)),
            vm((2, tok, slots), bf16), vm((n_ep, cap, feat), bf16),
            vm((rows, width), bf16), vm((rows, width), bf16), vm((rows, 1), f32),
            vm((rows, feat), f32), vm((rows + 8, feat), f32), vm((8, feat), f32),
            vm((rows, feat), bf16),
            vm((n_tp, rows, feat), bf16), vm((chips, rows, feat), bf16),
            vm((chips, rows, feat), bf16), vm((chips, rows, feat), bf16),
            vm((n_ep, cap, width), bf16), vm((slots, width), bf16), vm((slots, 1), f32),
            vm((slots, hidden), bf16),
            vm((n_tp, n_ep, cap, feat), bf16), vm((chips, n_ep, cap, feat), bf16),
            vm((chips, n_ep, cap, feat), bf16), vm((chips, n_ep, cap, feat), bf16),
            vm((n_ep, cap, feat), bf16), vm((n_ep, cap, feat), bf16),
            sem((chips,)), sem((chips,)), sem((chips,)), sem((chips,)),
            sem((n_ep,)), sem((n_ep,)),
            sem((chips, n_group)), sem((chips, n_group)),
            sem((chips, n_group)), sem((chips, n_group)),
            sem((2,)),
            sem((chips,)), sem((chips,)), sem((chips,)), sem((chips,)),
            sem((chips,)), sem((chips,)),
            sem((chips, n_group)), sem((chips, n_group)),
            sem((n_ep,)), sem((n_ep,)),
        ]
        v = pl.BlockSpec(memory_space=pltpu.VMEM)
        a = pl.BlockSpec(memory_space=pl.ANY)
        return pl.pallas_call(
            functools.partial(kernel, (n_ep, n_tp, cap, group)),
            out_shape=(
                jax.ShapeDtypeStruct((rows, feat), bf16),
                jax.ShapeDtypeStruct((tok, feat), bf16),
            ),
            in_specs=[v, v, a, a, a, v, a, v, v, v, v, a, a, a],
            out_specs=(v, v),
            scratch_shapes=scratch,
            compiler_params=pltpu.CompilerParams(
                collective_id=0, has_side_effects=True, vmem_limit_bytes=62 << 20
            ),
        )(
            mix_input, mix_gain.reshape(1, -1), gate_b, gate_c, value_w, conv_weight, out_weight,
            expert_input, expert_gain.reshape(1, -1), routes, route_weight,
            expert_gate, expert_up, expert_down.reshape(hidden, width),
        )

    in_specs = (
        P("ep", "tp"), P(), P(None, "tp"), P(None, "tp"), P(None, "tp"), P(None, "tp"),
        P("tp", None), P("ep", "tp"), P(), P("ep", None), P("ep", None),
        P("ep", None, "tp"), P("ep", None, "tp"), P("ep", "tp", None),
    )
    out_specs = (P("ep", "tp"), P("ep", "tp"))
    return jax.shard_map(local, mesh=mesh, in_specs=in_specs, out_specs=out_specs, check_vma=False)
```

```python
import functools

import jax
import jax.numpy as jnp
from jax import lax
from jax.experimental import pallas as pl
from jax.experimental.pallas import tpu as pltpu
from jax.sharding import PartitionSpec as P

MESH = pl.DeviceIdType.MESH
epsilon = 1e-06
routed_scale = 2.5
f32 = jnp.float32
bf16 = jnp.bfloat16


def kernel(
    dims,
    mix_ref, mgain_ref, wb_hbm, wc_hbm, wv_hbm, conv_ref, wo_hbm,
    exp_ref, egain_ref, routes_ref, rw_ref, wg_hbm, wu_hbm, wd_hbm,
    mo_ref, eo_ref,
    wb, wc, wv, wo, wg, wu, wd, w_sem,
    tables, outg, xg, xs, fac, outer, prod, edge, gated, pm, rm, sm, ym,
    xe, xes, efac, act, pe, re, se, yr, fin, ret,
    mys, myr, mps, mpr, eps, epr, eys, eyr, pps, ppr, edges,
    rms, rmr, yms, ymr, res, rer, ses, ser, rts, rtr,
):
    n_ep, n_tp, cap, group = dims
    chips = n_tp // 2
    n_group = n_ep // group
    rows, feat = mix_ref.shape
    width = feat * n_tp
    tok = exp_ref.shape[0]
    slots = n_ep * cap
    half = n_ep // 2
    e = lax.axis_index("ep")
    t = lax.axis_index("tp")
    y, c = lax.div(t, 2), lax.rem(t, 2)
    partner = y * 2 + 1 - c
    home = lax.div(e, group)

    def cols(b):
        return pl.ds(pl.multiple_of(b * feat, feat), feat)

    def remote(src, dst, send_sem, recv_sem, ep, tp):
        return pltpu.make_async_remote_copy(
            src_ref=src, dst_ref=dst, send_sem=send_sem, recv_sem=recv_sem,
            device_id=(ep, tp), device_id_type=MESH,
        )

    def ahead(dy):
        return lax.rem(y + dy, chips) * 2 + c

    def behind(dy):
        return lax.rem(y - dy + chips, chips) * 2 + c

    def loop(count, body, start=0):
        lax.fori_loop(start, count, lambda i, carry: (body(i), carry)[1], 0)

    def mix_y(dy):
        return remote(mix_ref, xg.at[:, cols(t)], mys.at[dy], myr.at[dy], e, ahead(dy))

    def mix_p():
        return remote(mix_ref, xg.at[:, cols(t)], mps.at[0], mpr.at[0], e, partner)

    def mix_f(dy):
        part = xg.at[:, cols(behind(dy))]
        return remote(part, part, mps.at[dy], mpr.at[dy], e, partner)

    def dispatch(d):
        s = lax.rem(e + d, n_ep)
        return remote(outg.at[s], xe.at[e, :, cols(t)], eps.at[d], epr.at[d], s, t)

    def span_in(i):
        return pl.ds(lax.rem(home - i + n_group, n_group) * group, group)

    def exp_y(i, dy):
        part = xe.at[span_in(i), :, cols(t)]
        return remote(part, part, eys.at[dy, i], eyr.at[dy, i], e, ahead(dy))

    def exp_p(i):
        part = xe.at[span_in(i), :, cols(t)]
        return remote(part, part, pps.at[0, i], ppr.at[0, i], e, partner)

    def exp_f(i, dy):
        part = xe.at[span_in(i), :, cols(behind(dy))]
        return remote(part, part, pps.at[dy, i], ppr.at[dy, i], e, partner)

    def edge_copy():
        return remote(
            prod.at[pl.ds(rows, 8)], edge, edges.at[0], edges.at[1], lax.rem(e + 1, n_ep), t
        )

    def mix_half(q):
        return remote(pm.at[q * 2 + 1 - c], rm.at[q], rms.at[q], rmr.at[q], e, partner)

    def mix_sum(dy):
        return remote(sm.at[dy], ym.at[dy], yms.at[dy], ymr.at[dy], e, ahead(dy))

    def exp_half(q, h):
        at = pl.ds(h * half, half)
        return remote(
            pe.at[q * 2 + 1 - c, at], re.at[q, at], res.at[h, q], rer.at[h, q], e, partner
        )

    def span_out(i):
        return pl.ds(i * group, group)

    def source(p):
        return lax.rem(home - lax.div(p, group) + n_group, n_group) * group + lax.rem(p, group)

    def place(s):
        turn = lax.rem(home - lax.div(s, group) + n_group, n_group)
        return turn * group + lax.rem(s, group)

    def exp_sum(i, dy):
        return remote(
            se.at[dy, span_out(i)], yr.at[dy, span_out(i)],
            ses.at[dy, i], ser.at[dy, i], e, ahead(dy),
        )

    def back(d):
        s = lax.rem(e + d, n_ep)
        return remote(fin.at[place(s)], ret.at[e], rts.at[d], rtr.at[d], s, t)

    loads = [
        pltpu.make_async_copy(src, dst, w_sem.at[i])
        for i, (src, dst) in enumerate(
            ((wb_hbm, wb), (wc_hbm, wc), (wv_hbm, wv), (wo_hbm, wo),
             (wg_hbm, wg), (wu_hbm, wu), (wd_hbm, wd))
        )
    ]
    for load in loads:
        load.start()

    barrier = pltpu.get_barrier_semaphore()
    for dy in range(1, chips):
        pl.semaphore_signal(barrier, inc=1, device_id=(e, ahead(dy)), device_id_type=MESH)
    pl.semaphore_signal(barrier, inc=1, device_id=(e, partner), device_id_type=MESH)

    def greet(d):
        pl.semaphore_signal(
            barrier, inc=1, device_id=(lax.rem(e + d + 1, n_ep), t), device_id_type=MESH
        )

    loop(n_ep - 1, greet)

    row = lax.broadcasted_iota(jnp.int32, (tok, tok), 0)
    column = lax.broadcasted_iota(jnp.int32, (tok, tok), 1)

    def upright(line):
        return jnp.sum(jnp.where(row == column, line, 0.0), axis=1, keepdims=True)

    lane = lax.broadcasted_iota(jnp.int32, (tok, 128), 1).astype(f32)
    chosen = [upright(routes_ref[k : k + 1, :].astype(f32)) for k in range(2)]
    named = [chosen[k] == lane for k in range(2)]
    either = jnp.where(named[0] | named[1], 1.0, 0.0).astype(bf16)
    before = row > column
    counts = jnp.dot(
        jnp.where(before, 1.0, 0.0).astype(bf16), either, preferred_element_type=f32
    )
    slot_iota = lax.broadcasted_iota(jnp.int32, (tok, slots), 1).astype(f32)
    both = []
    for k in range(2):
        rank = jnp.sum(jnp.where(named[k], counts, 0.0), axis=1, keepdims=True)
        slot = chosen[k] * float(cap) + rank
        one = jnp.where(slot_iota == slot, 1.0, 0.0)
        tables[k] = one.astype(bf16)
        both.append(one)
    send = (both[0] + both[1]).astype(bf16)
    outg[...] = (
        lax.dot_general(
            send, exp_ref[...], (((0,), (0,)), ((), ())), preferred_element_type=f32
        )
        .astype(bf16)
        .reshape(n_ep, cap, feat)
    )

    pl.semaphore_wait(barrier, n_ep - 1 + chips)

    loop(n_ep - 1, lambda d: dispatch(d + 1).start())
    for dy in range(1, chips):
        mix_y(dy).start()
    mix_p().start()
    xe[e, :, cols(t)] = outg[e]
    xg[:, cols(t)] = mix_ref[...]

    def pass_on(i):
        first = lax.rem(home - i + n_group, n_group) * group
        for j in range(group):
            d = lax.rem(e - first - j + n_ep, n_ep)

            @pl.when(d != 0)
            def _():
                dispatch(d).wait_recv()

        for dy in range(1, chips):
            exp_y(i, dy).start()
        exp_p(i).start()

    early = n_group * 5 // 8
    loop(early, pass_on)

    for dy in range(1, chips):
        mix_y(dy).wait_recv()
        mix_f(dy).start()
    mix_p().wait_recv()
    for dy in range(1, chips):
        mix_f(dy).wait_recv()

    tile = 32

    def scale_mix(i):
        at = pl.ds(pl.multiple_of(i * tile, tile), tile)
        x = xg[at].astype(f32)
        fac[at] = lax.rsqrt(jnp.sum(x * x, axis=1, keepdims=True) / width + epsilon)
        xs[at] = (x * mgain_ref[...]).astype(bf16)

    loop(rows // tile, scale_mix)
    for load in loads[:3]:
        load.wait()
    wide = 256 if feat % 256 == 0 else feat

    def project(i):
        at = pl.ds(pl.multiple_of(i * wide, wide), wide)
        x = xs[...]
        factor = fac[...]
        inner = jnp.dot(x, wc[:, at], preferred_element_type=f32) * factor
        values = jnp.dot(x, wv[:, at], preferred_element_type=f32) * factor
        prod[pl.ds(8, rows), at] = inner * values
        outer[:, at] = jnp.dot(x, wb[:, at], preferred_element_type=f32) * factor

    loop(feat // wide, project)
    edge_copy().start()
    loop(n_group, pass_on, early)

    def relay(i):
        for dy in range(1, chips):
            exp_y(i, dy).wait_recv()
            exp_f(i, dy).start()

    def arrive(i):
        exp_p(i).wait_recv()
        for dy in range(1, chips):
            exp_f(i, dy).wait_recv()

    def scale_exp(p):
        at = pl.ds(pl.multiple_of(p * cap, cap), cap)
        x = xe[source(p)].astype(f32)
        efac[at] = lax.rsqrt(jnp.sum(x * x, axis=1, keepdims=True) / width + epsilon)
        xes[at] = (x * egain_ref[...]).astype(bf16)

    hidden = wd.shape[0]
    wide_h = 256 if hidden % 256 == 0 else hidden

    def push(i):
        at = span_out(i)
        for dy in range(1, chips):
            q = lax.rem(y + dy, chips)
            se[dy, at] = (pe[ahead(dy), at].astype(f32) + re[q, at].astype(f32)).astype(bf16)
            exp_sum(i, dy).start()

    for h in range(2):
        first, last = h * n_group // 2, (h + 1) * n_group // 2
        loop(last, relay, first)
        loop(last, arrive, first)
        loop((h + 1) * half, scale_exp, h * half)
        if h == 0:
            loads[4].wait()
            loads[5].wait()
        part = pl.ds(h * half * cap, half * cap)

        def activate(at):
            x = xes[part]
            factor = efac[part]
            gate = jnp.dot(x, wg[0, :, at], preferred_element_type=f32) * factor
            up = jnp.dot(x, wu[0, :, at], preferred_element_type=f32) * factor
            act[part, at] = (gate / (1.0 + jnp.exp(-gate)) * up).astype(bf16)

        if wide_h == hidden:
            activate(slice(None))
        else:
            loop(
                hidden // wide_h,
                lambda i: activate(pl.ds(pl.multiple_of(i * wide_h, wide_h), wide_h)),
            )
        if h == 0:
            loads[6].wait()

        def exp_down(b):
            out = jnp.dot(act[part], wd[:, cols(b)], preferred_element_type=f32)
            pe[b, pl.ds(h * half, half)] = out.astype(bf16).reshape(half, cap, feat)

        def exp_given(q):
            exp_down(q * 2 + 1 - c)
            exp_half(q, h).start()

        loop(chips, exp_given)
        loop(chips, lambda q: exp_down(q * 2 + c))
        for q in range(chips):
            exp_half(q, h).wait_recv()
        loop(last, push, first)

    edge_copy().wait_recv()
    prod[0:8] = jnp.where(e == 0, 0.0, edge[...])

    def convolve(i):
        at = pl.ds(pl.multiple_of(i * 128, 128), 128)
        convolved = (
            conv_ref[0:1, at] * prod[pl.ds(6, rows), at]
            + conv_ref[1:2, at] * prod[pl.ds(7, rows), at]
            + conv_ref[2:3, at] * prod[pl.ds(8, rows), at]
        )
        gated[:, at] = (outer[:, at] * convolved).astype(bf16)

    loop(feat // 128, convolve)
    loads[3].wait()

    def mix_down(b):
        pm[b] = jnp.dot(gated[...], wo[:, cols(b)], preferred_element_type=f32).astype(bf16)

    def mix_given(q):
        mix_down(q * 2 + 1 - c)
        mix_half(q).start()

    loop(chips, mix_given)
    loop(chips, lambda q: mix_down(q * 2 + c))
    for q in range(chips):
        mix_half(q).wait_recv()
    for dy in range(1, chips):
        q = lax.rem(y + dy, chips)
        sm[dy] = (pm[ahead(dy)].astype(f32) + rm[q].astype(f32)).astype(bf16)
        mix_sum(dy).start()

    def finish(i):
        at = span_out(i)
        whole = pe[t, at].astype(f32) + re[y, at].astype(f32)
        for dy in range(1, chips):
            exp_sum(i, dy).wait_recv()
            whole = whole + yr[dy, at].astype(f32)
        fin[at] = whole.astype(bf16)
        first = lax.rem(home - i + n_group, n_group) * group
        for j in range(group):
            d = lax.rem(first + j - e + n_ep, n_ep)

            @pl.when(d != 0)
            def _():
                back(d).start()

    loop(n_group, finish)
    ret[e] = fin[place(e)]
    loop(n_ep - 1, lambda d: back(d + 1).wait_recv())

    scores = rw_ref[...]
    normalized = scores / jnp.sum(scores, axis=0, keepdims=True) * routed_scale
    share = [upright(normalized[k : k + 1, :]) for k in range(2)]
    results = ret[...].reshape(slots, feat)
    eo_ref[...] = (
        share[0] * jnp.dot(tables[0], results, preferred_element_type=f32)
        + share[1] * jnp.dot(tables[1], results, preferred_element_type=f32)
    ).astype(bf16)

    total = pm[t].astype(f32) + rm[y].astype(f32)
    for dy in range(1, chips):
        mix_sum(dy).wait_recv()
        total = total + ym[dy].astype(f32)
    mo_ref[...] = total.astype(bf16)

    def drain(d):
        dispatch(d + 1).wait_send()
        back(d + 1).wait_send()

    loop(n_ep - 1, drain)
    mix_p().wait_send()
    edge_copy().wait_send()
    for dy in range(1, chips):
        mix_y(dy).wait_send()
        mix_f(dy).wait_send()
        mix_sum(dy).wait_send()
    for q in range(chips):
        mix_half(q).wait_send()
        exp_half(q, 0).wait_send()
        exp_half(q, 1).wait_send()

    def drain_groups(i):
        exp_p(i).wait_send()
        for dy in range(1, chips):
            exp_y(i, dy).wait_send()
            exp_f(i, dy).wait_send()
            exp_sum(i, dy).wait_send()

    loop(n_group, drain_groups)


def solution(mesh):
    n_ep, n_tp = mesh.shape["ep"], mesh.shape["tp"]
    chips = n_tp // 2

    def local(
        mix_input, mix_gain, gate_b, gate_c, value_w, conv_weight, out_weight,
        expert_input, expert_gain, routes, route_weight, expert_gate, expert_up, expert_down,
    ):
        rows, feat = mix_input.shape
        width = feat * n_tp
        tok, top = routes.shape
        experts = n_ep * expert_gate.shape[0]
        assert expert_gate.shape[0] == 1 and top == 2
        cap = -(-(2 * tok * top // experts) // 16) * 16
        hidden = expert_gate.shape[2]
        group = max(1, n_ep // 8)
        n_group = n_ep // group
        slots = n_ep * cap
        vm, sem = pltpu.VMEM, pltpu.SemaphoreType.DMA
        scratch = [
            vm((width, feat), bf16), vm((width, feat), bf16), vm((width, feat), bf16),
            vm((feat, width), bf16),
            vm((1, width, hidden), bf16), vm((1, width, hidden), bf16), vm((hidden, width), bf16),
            sem((7,)),
            vm((2, tok, slots), bf16), vm((n_ep, cap, feat), bf16),
            vm((rows, width), bf16), vm((rows, width), bf16), vm((rows, 1), f32),
            vm((rows, feat), f32), vm((rows + 8, feat), f32), vm((8, feat), f32),
            vm((rows, feat), bf16),
            vm((n_tp, rows, feat), bf16), vm((chips, rows, feat), bf16),
            vm((chips, rows, feat), bf16), vm((chips, rows, feat), bf16),
            vm((n_ep, cap, width), bf16), vm((slots, width), bf16), vm((slots, 1), f32),
            vm((slots, hidden), bf16),
            vm((n_tp, n_ep, cap, feat), bf16), vm((chips, n_ep, cap, feat), bf16),
            vm((chips, n_ep, cap, feat), bf16), vm((chips, n_ep, cap, feat), bf16),
            vm((n_ep, cap, feat), bf16), vm((n_ep, cap, feat), bf16),
            sem((chips,)), sem((chips,)), sem((chips,)), sem((chips,)),
            sem((n_ep,)), sem((n_ep,)),
            sem((chips, n_group)), sem((chips, n_group)),
            sem((chips, n_group)), sem((chips, n_group)),
            sem((2,)),
            sem((chips,)), sem((chips,)), sem((chips,)), sem((chips,)),
            sem((2, chips)), sem((2, chips)),
            sem((chips, n_group)), sem((chips, n_group)),
            sem((n_ep,)), sem((n_ep,)),
        ]
        v = pl.BlockSpec(memory_space=pltpu.VMEM)
        a = pl.BlockSpec(memory_space=pl.ANY)
        return pl.pallas_call(
            functools.partial(kernel, (n_ep, n_tp, cap, group)),
            out_shape=(
                jax.ShapeDtypeStruct((rows, feat), bf16),
                jax.ShapeDtypeStruct((tok, feat), bf16),
            ),
            in_specs=[v, v, a, a, a, v, a, v, v, v, v, a, a, a],
            out_specs=(v, v),
            scratch_shapes=scratch,
            compiler_params=pltpu.CompilerParams(
                collective_id=0, has_side_effects=True, vmem_limit_bytes=62 << 20
            ),
        )(
            mix_input, mix_gain.reshape(1, -1), gate_b, gate_c, value_w, conv_weight, out_weight,
            expert_input, expert_gain.reshape(1, -1), routes.T, route_weight.T,
            expert_gate, expert_up, expert_down.reshape(hidden, width),
        )

    in_specs = (
        P("ep", "tp"), P(), P(None, "tp"), P(None, "tp"), P(None, "tp"), P(None, "tp"),
        P("tp", None), P("ep", "tp"), P(), P("ep", None), P("ep", None),
        P("ep", None, "tp"), P("ep", None, "tp"), P("ep", "tp", None),
    )
    out_specs = (P("ep", "tp"), P("ep", "tp"))
    return jax.shard_map(local, mesh=mesh, in_specs=in_specs, out_specs=out_specs, check_vma=False)
```
